32 devices in a mesh: sp: 8 (over z, core), tp: 4 (over y, x).
Axes of the slice: x: 2, y: 2, z: 4, core: 2. Of those that a mesh axis runs over, the one named last changes fastest.
Arguments:
- cotangent: bfloat16 [1024, 2048], P('sp', 'tp'), may hold values from -3 to 3
- moe_input: bfloat16 [1024, 2048], P('sp', 'tp'), may hold values from -6 to 6
- expert_ids: int32 [1024, 2], P('sp'), may hold values from 0 to 7, all different within a row; in each aligned block of 128 rows (0 to 127, 128 to 255, ...) at most 48 rows name the same one
- group_gate: float32 [1024], P('sp'), may hold values from 0.3 to 1
- expert_gate: float32 [1024, 2], P('sp'), may hold values from 0.1 to 0.9
- weight_gate: bfloat16 [8, 2048, 512], P('sp', None, 'tp'), may hold values from -0.125 to 0.125
- weight_up: bfloat16 [8, 2048, 512], P('sp', None, 'tp'), may hold values from -0.125 to 0.125
- weight_down: bfloat16 [8, 512, 2048], P('sp', 'tp'), may hold values from -0.25 to 0.25
- out_weight: bfloat16 [2048, 1024], P(None, 'tp'), may hold values from -0.1875 to 0.1875
- mixer_out: bfloat16 [1024, 1024], P('sp', 'tp'), may hold values from -6 to 6
- queries: bfloat16 [1024, 512], P('sp', 'tp'), may hold values from -6 to 6
- key_vectors: bfloat16 [1024, 512], P('sp', 'tp'), may hold values from -6 to 6
- values: bfloat16 [1024, 1024], P('sp', 'tp'), may hold values from -6 to 6
- log_decay: float32 [1024, 512], P('sp', 'tp'), may hold values from -0.9 to 0
Outputs:
- grad_gate: bfloat16 [8, 2048, 512], P('sp', None, 'tp')
- grad_up: bfloat16 [8, 2048, 512], P('sp', None, 'tp')
- grad_down: bfloat16 [8, 512, 2048], P('sp', 'tp')
- proj_grad: float32 [2048, 1024], P('sp', 'tp')
- grad_queries: bfloat16 [1024, 512], P('sp', 'tp')
- grad_keys: bfloat16 [1024, 512], P('sp', 'tp')
- grad_values: bfloat16 [1024, 1024], P('sp', 'tp')
- grad_decay: float32 [1024, 512], P('sp', 'tp')
The draws below stay inside these ranges and needn't reach their ends.
Inputs may be any that keep to these rules, and one draw needn't show every extreme that they name: `expert_ids`: in the rows of one index of sp no expert is named by more than 48 rows, a bound that some block reaches.
All inputs are finite; a program needn't handle non-finite values.
Results may differ from the reference program's by a relative error of at most 0.013.
Values may be sent and summed in bfloat16 or wider, within the bound.
A program may use at most 128 MiB of HBM per device.

```python
import math
import jax
import jax.numpy as jnp
import numpy as np
from jax import lax

D = 2048
DK = 128
DV = 256
HEADS = 4
KEY_CHANNELS = 512
VAL_WIDTH = 1024
FE_DEV = 128
FE = 512
EXPERTS = 8
TOK = 128
SEQUENCE_TOKENS = 1024
BLK = 64
CAP = 48
N_SP = 8
N_TP = 4


def draw_log_decay(key, part):
    random_subkeys = jax.random.split(jax.random.fold_in(key, 17), 7)
    fast_share = 0.5
    fast_channel_flag = jax.random.uniform(random_subkeys[0], (KEY_CHANNELS,)) < fast_share
    fast_rate = 2.3026 / jax.random.uniform(random_subkeys[1], (KEY_CHANNELS,), minval=30.0, maxval=100.0) / 2.0
    slow_rate = 0.4 / (4.5 * SEQUENCE_TOKENS) * jnp.exp(jax.random.uniform(random_subkeys[2], (KEY_CHANNELS,), minval=-2.3026, maxval=0.0))
    base_rate = jnp.where(fast_channel_flag, fast_rate, slow_rate)
    block_factor = jnp.exp(jax.random.uniform(random_subkeys[3], (SEQUENCE_TOKENS // TOK,), minval=0.0, maxval=1.0986))
    block_factor = jnp.repeat(block_factor, TOK)
    element_factor = jax.random.uniform(random_subkeys[4], (SEQUENCE_TOKENS, KEY_CHANNELS), minval=0.5, maxval=1.5)
    channel_decay_speed = base_rate[None, :] * block_factor[:, None] * element_factor
    spike_locations = jax.random.randint(random_subkeys[5], (2,), 0, SEQUENCE_TOKENS)
    spike_position = jnp.any(jnp.arange(SEQUENCE_TOKENS)[:, None] == spike_locations[None, :], axis=1)
    spike_penalty = jnp.log(jax.random.uniform(random_subkeys[6], (SEQUENCE_TOKENS, KEY_CHANNELS), minval=0.5, maxval=0.8))
    spike_events = jnp.where(spike_position[:, None] & jnp.logical_not(fast_channel_flag)[None, :], spike_penalty, 0.0)
    return (spike_events - channel_decay_speed).astype(jnp.float32)


def with_spikes(result, own_key, source, target, blocks, factor):
    owner, partner = [(jnp.arange(result.shape[axis_at]) // (result.shape[axis_at] // blocks)).reshape([-1 if axis == axis_at else 1 for axis in range(result.ndim)]) for axis_at in (source, target)]
    chosen = jax.random.permutation(own_key, blocks)[partner]
    strong = (owner == chosen) | (owner == (partner + blocks // 2) % blocks)
    return jnp.where(strong, factor * result, result)


def level_of(own_key, shape, cuts, low, top_value):
    factor_of, own = 1.0, jax.random.fold_in(own_key, 6)
    for dim, shards_of in cuts:
        steps = jnp.exp(jax.random.uniform(jax.random.fold_in(own, dim), (shards_of,), jnp.float32, low / len(cuts), top_value / len(cuts)))
        factor_of = factor_of * jnp.repeat(steps, shape[dim] // shards_of).reshape([-1 if axis == dim else 1 for axis in range(len(shape))])
    return factor_of


def assign_block(rng, own, number, rows, amount, top, reach, skew):
    sequence = jax.random.permutation(rng, amount)
    heavy_load, ordinary = shares(amount, rows * top, reach, skew, True), shares(amount, rows * top, reach, skew, False)
    places = jnp.arange(amount)

    def named(tallies, offset_by):
        used = int((tallies > 0).sum())
        fixed = max(1, used // 4)
        shifted = fixed + (places - fixed + offset_by * (used - fixed)) % max(1, amount - fixed)
        return jnp.zeros((amount,), jnp.int32).at[sequence[jnp.where(places < fixed, places, shifted)]].set(jnp.asarray(tallies, jnp.int32))

    tallies = jnp.where(number % 4 == 0, named(heavy_load, number // 4), named(ordinary, number - number // 4 - 1))
    mixed = jax.random.permutation(jax.random.fold_in(own, 3), amount)
    donor, taker = mixed[0:amount // 2 * 2:2], mixed[1:amount // 2 * 2:2]
    margin = jnp.minimum(tallies[donor] - 1, reach - tallies[taker]) // 2
    margin = jnp.where((donor == sequence[0]) | (taker == sequence[0]) | (tallies[taker] == 0), 0, jnp.maximum(margin, 0))
    shifted = jax.random.randint(jax.random.fold_in(own, 4), (amount // 2,), 0, 1 << 20) % (margin + 1)
    tallies = tallies.at[donor].add(-shifted).at[taker].add(shifted)
    members = jnp.searchsorted(jnp.cumsum(tallies), jnp.arange(rows * top), side="right").astype(jnp.int32)
    grid = members.reshape(top, rows).T
    grid = grid[jax.random.permutation(jax.random.fold_in(own, 1), rows)]
    offset_by = jax.random.randint(jax.random.fold_in(own, 2), (rows, 1), 0, top)
    return jnp.take_along_axis(grid, (jnp.arange(top)[None, :] + offset_by) % top, axis=1)


def shares(count, total, bound, skew, full):
    portions = [(1 << 20) // math.isqrt(grade ** skew) + 1 for grade in range(1, count + 1)]
    largest = bound if full else min(bound, max(-(-total // count), total * portions[0] // sum(portions)))
    least = 1 if total - largest >= count - 1 else 0
    counts, spare = [largest] + [least] * (count - 1), total - largest - least * (count - 1)
    while spare > 0:
        movable = [i for i in range(1, count) if counts[i] < largest] or [i for i in range(1, count) if counts[i] < bound]
        whole, budget = sum([portions[i] for i in movable]), spare
        for i in movable:
            addition = min(bound - counts[i], max(1, budget * portions[i] // whole), spare)
            counts[i] = counts[i] + addition
            spare = spare - addition
    return np.array(counts)


def normal_values(rng, shape, width, most, cuts=(), kind=jnp.bfloat16):
    level = level_of(rng, shape, cuts, -0.22, 0.18) if cuts else 1.0
    drawn = jax.random.normal(rng, shape, jnp.float32) * width * level
    return jnp.minimum(jnp.maximum(drawn, -most), most).astype(kind)


def heavy_noise(key, shape, width, bound, cuts, heavy, held_as=jnp.bfloat16):
    values = width * jax.random.normal(key, shape, jnp.float32)
    if cuts:
        values = values * level_of(key, shape, cuts, -0.22, 0.18)
    return jnp.clip(with_spikes(values, jax.random.fold_in(key, 3), *heavy), -bound, bound).astype(held_as)


def setup_inputs(seed: int = 0) -> dict:
    key_of = jax.random.split(jax.random.key(seed), 15)
    cotangent = heavy_noise(key_of[0], (SEQUENCE_TOKENS, D), 0.5, 3.0, ((0, 8), (1, 4)), (0, 1, 8, 2.0))
    moe_input = normal_values(key_of[1], (SEQUENCE_TOKENS, D), 1.0, 6.0, ((0, 8), (1, 4)))
    expert_ids_keys = jax.random.split(jax.random.fold_in(key_of[2], 1), SEQUENCE_TOKENS // TOK)
    expert_ids_turns = jax.random.permutation(jax.random.fold_in(key_of[2], 3), SEQUENCE_TOKENS // TOK)
    expert_ids = jax.vmap(lambda own, number: assign_block(jax.random.fold_in(key_of[2], 2), own, number, TOK, EXPERTS, 2, CAP, 2))(expert_ids_keys, expert_ids_turns).reshape((SEQUENCE_TOKENS, 2))
    group_gate = jnp.clip(0.3 + 0.7 * jax.random.uniform(key_of[3], (SEQUENCE_TOKENS,), jnp.float32) ** level_of(key_of[3], (SEQUENCE_TOKENS,), ((0, 8),), -0.2, 0.2), 0.3, 1.0)
    expert_gate = jnp.clip(0.1 + 0.79999997 * jax.random.uniform(key_of[4], (SEQUENCE_TOKENS, 2), jnp.float32) ** level_of(key_of[4], (SEQUENCE_TOKENS, 2), ((0, 8),), -0.2, 0.2), 0.1, 0.9)
    weight_gate = normal_values(key_of[5], (EXPERTS, D, FE), D ** -0.5, 0.125, ((0, 8), (2, 4)))
    weight_up = normal_values(key_of[6], (EXPERTS, D, FE), D ** -0.5, 0.125, ((0, 8), (2, 4)))
    weight_down = normal_values(key_of[7], (EXPERTS, FE, D), FE ** -0.5, 0.25, ((0, 8), (1, 4)))
    out_weight = normal_values(key_of[8], (D, VAL_WIDTH), VAL_WIDTH ** -0.5, 0.1875, ((1, 4),))
    mixer_out = normal_values(key_of[9], (SEQUENCE_TOKENS, VAL_WIDTH), 1.0, 6.0, ((0, 8), (1, 4)))
    queries = normal_values(key_of[10], (SEQUENCE_TOKENS, KEY_CHANNELS), 1.0, 6.0, ((0, 8), (1, 4)))
    key_vectors = normal_values(key_of[11], (SEQUENCE_TOKENS, KEY_CHANNELS), 1.0, 6.0, ((0, 8), (1, 4)))
    values = normal_values(key_of[12], (SEQUENCE_TOKENS, VAL_WIDTH), 1.0, 6.0, ((0, 8), (1, 4)))
    log_decay = draw_log_decay(jax.random.fold_in(key_of[14], 71), 0)
    return {"cotangent": cotangent, "moe_input": moe_input, "expert_ids": expert_ids, "group_gate": group_gate, "expert_gate": expert_gate, "weight_gate": weight_gate, "weight_up": weight_up, "weight_down": weight_down, "out_weight": out_weight, "mixer_out": mixer_out, "queries": queries, "key_vectors": key_vectors, "values": values, "log_decay": log_decay}


HIGHEST = lax.Precision.HIGHEST

def local_forward(query_heads, key_heads, value_heads, decay_heads, state_in):
    head_count, row_count = (query_heads.shape[0], query_heads.shape[1])
    block_count = row_count // BLK
    causal = jnp.tril(jnp.ones((BLK, BLK), dtype=bool))
    causal_wide = causal[None, :, :, None]

    def blocked(tensor):
        return jnp.moveaxis(tensor.reshape(head_count, block_count, BLK, tensor.shape[-1]), 1, 0)

    def block_step(running, pieces):
        query_blk, key_blk, value_blk, decay_blk = pieces
        cumulative = jnp.cumsum(decay_blk, axis=1)
        block_end = cumulative[:, -1:, :]
        query_scaled = query_blk * DK ** (-0.5)
        query_dec = query_scaled * jnp.exp(cumulative)
        key_end = key_blk * jnp.exp(block_end - cumulative)
        spread = jnp.where(causal_wide, cumulative[:, :, None, :] - cumulative[:, None, :, :], 0.0)
        pair_decay = jnp.where(causal_wide, jnp.exp(spread), 0.0)
        scores = jnp.einsum('hcd,hsd,hcsd->hcs', query_scaled, key_blk, pair_decay, precision=HIGHEST)
        outputs = jnp.einsum('hcs,hsv->hcv', scores, value_blk, precision=HIGHEST)
        outputs = outputs + jnp.einsum('hcd,hdv->hcv', query_dec, running, precision=HIGHEST)
        running = jnp.exp(block_end[:, 0, :])[:, :, None] * running + jnp.einsum('hcd,hcv->hdv', key_end, value_blk, precision=HIGHEST)
        return (running, outputs)
    state_out, outputs = lax.scan(block_step, state_in, (blocked(query_heads), blocked(key_heads), blocked(value_heads), blocked(decay_heads)))
    return (jnp.moveaxis(outputs, 0, 1).reshape(head_count, row_count, -1), state_out)

def heads_first(tensor, width_in):
    return tensor.astype(jnp.float32).reshape(tensor.shape[0], -1, width_in).transpose(1, 0, 2)

def tokens_first(tensor):
    return tensor.transpose(1, 0, 2).reshape(tensor.shape[1], -1)

def expert_back(routed, inputs, w_gate, w_up, w_down):
    gate_pre = jnp.dot(inputs, w_gate, preferred_element_type=jnp.float32)
    up_pre = jnp.dot(inputs, w_up, preferred_element_type=jnp.float32)
    sigmoid_g = jax.nn.sigmoid(gate_pre)
    active = gate_pre * sigmoid_g
    hidden = (active * up_pre).astype(jnp.bfloat16)
    back_grad = lax.dot_general(routed, w_down, (((1,), (1,)), ((), ())), preferred_element_type=jnp.float32)
    d_up = (back_grad * active).astype(jnp.bfloat16)
    d_gate = (back_grad * up_pre * sigmoid_g * (1.0 + gate_pre * (1.0 - sigmoid_g))).astype(jnp.bfloat16)
    contract = (((0,), (0,)), ((), ()))
    grad_down = lax.dot_general(hidden, routed, contract, preferred_element_type=jnp.float32).astype(jnp.bfloat16)
    grad_gate = lax.dot_general(inputs, d_gate, contract, preferred_element_type=jnp.float32).astype(jnp.bfloat16)
    grad_up = lax.dot_general(inputs, d_up, contract, preferred_element_type=jnp.float32).astype(jnp.bfloat16)
    return (grad_gate, grad_up, grad_down, d_gate, d_up)

def reference(cotangent, moe_input, expert_ids, group_gate, expert_gate, weight_gate, weight_up, weight_down, out_weight, mixer_out, queries, key_vectors, values, log_decay):
    slot_limit = N_SP * CAP
    route_weight = group_gate[:, None] * expert_gate
    positions = jnp.arange(slot_limit, dtype=jnp.int32)

    def per_expert(accumulated, inputs):
        expert_index, w_gate, w_up, w_down = inputs
        member = expert_ids == expert_index
        chosen = jnp.any(member, axis=1)
        route_share = lax.optimization_barrier(jnp.sum(jnp.where(member, route_weight, 0.0), axis=1))
        row_ids = jnp.nonzero(chosen, size=slot_limit, fill_value=0)[0].astype(jnp.int32)
        is_valid = (positions < jnp.sum(chosen.astype(jnp.int32)))[:, None]
        routed = jnp.where(is_valid, route_share[row_ids][:, None] * cotangent[row_ids].astype(jnp.float32), 0.0).astype(jnp.bfloat16)
        rows_in = jnp.where(is_valid, moe_input[row_ids], jnp.zeros((), jnp.bfloat16))
        grad_gate, grad_up, grad_down, d_gate, d_up = expert_back(routed, rows_in, w_gate, w_up, w_down)
        split_gate = d_gate.astype(jnp.float32).reshape(slot_limit, N_TP, FE_DEV)
        split_up = d_up.astype(jnp.float32).reshape(slot_limit, N_TP, FE_DEV)
        partials = jnp.einsum('cjf,djf->jcd', split_gate, w_gate.astype(jnp.float32).reshape(D, N_TP, FE_DEV), precision=HIGHEST)
        partials = partials + jnp.einsum('cjf,djf->jcd', split_up, w_up.astype(jnp.float32).reshape(D, N_TP, FE_DEV), precision=HIGHEST)
        rounded = lax.optimization_barrier(partials.astype(jnp.bfloat16))
        summed = lax.optimization_barrier(lax.optimization_barrier(jnp.sum(rounded.astype(jnp.float32), axis=0)).astype(jnp.bfloat16))
        accumulated = accumulated.at[row_ids].add(jnp.where(is_valid, summed.astype(jnp.float32), 0.0))
        return (accumulated, (grad_gate, grad_up, grad_down))
    accumulated, grads = lax.scan(per_expert, jnp.zeros((SEQUENCE_TOKENS, D), jnp.float32), (jnp.arange(EXPERTS, dtype=jnp.int32), weight_gate, weight_up, weight_down))
    residual_grad = (cotangent.astype(jnp.float32) + accumulated).astype(jnp.bfloat16)
    grad_mix = jnp.dot(residual_grad, out_weight, preferred_element_type=jnp.float32).astype(jnp.bfloat16)
    proj_grad = lax.dot_general(residual_grad, mixer_out, (((0,), (0,)), ((), ())), preferred_element_type=jnp.float32)
    state_zero = jnp.zeros((HEADS, DK, DV), jnp.float32)

    def whole_forward(query_heads, key_heads, value_heads, decay_heads):
        return local_forward(query_heads, key_heads, value_heads, decay_heads, state_zero)
    primal, pullback = jax.vjp(whole_forward, heads_first(queries, DK), heads_first(key_vectors, DK), heads_first(values, DV), heads_first(log_decay, DK))
    grad_q, grad_k, grad_v, grad_l = pullback((heads_first(grad_mix, DV), jnp.zeros_like(state_zero)))
    return (grads[0], grads[1], grads[2], proj_grad, tokens_first(grad_q).astype(jnp.bfloat16), tokens_first(grad_k).astype(jnp.bfloat16), tokens_first(grad_v).astype(jnp.bfloat16), tokens_first(grad_l))
```

```python
import functools
import math

import jax
import jax.numpy as jnp
from jax import lax
from jax.experimental import pallas as pl
from jax.experimental.pallas import tpu as pltpu
from jax.sharding import PartitionSpec as P

DK = 128
DV = 256
TOK = 128
BLK = 64
HIGHEST = lax.Precision.HIGHEST
F32 = jnp.float32
BF16 = jnp.bfloat16
MESH = pl.DeviceIdType.MESH


def tp_grid(n_tp):
    cols = math.isqrt(n_tp)
    while n_tp % cols:
        cols -= 1
    return n_tp // cols, cols


def sp_order(n_sp):
    if n_sp % 2:
        return [(d, 0) for d in range(1, n_sp)], n_sp, 1
    z = n_sp // 2
    places = [(dz, dc) for dz in range(z) for dc in range(2)][1:]
    places.sort(key=lambda p: (min(p[0], z - p[0]), p))
    return places, z, 2


class Place:
    def __init__(self, n_sp, n_tp):
        self.n_sp, self.n_tp = n_sp, n_tp
        self.sp, self.tp = lax.axis_index("sp"), lax.axis_index("tp")
        self.order, self.z, self.cores = sp_order(n_sp)
        self.rows, self.cols = tp_grid(n_tp)

    def sp_peer(self, place, back=False):
        dz, dc = place
        zz, cc = self.sp // self.cores, self.sp % self.cores
        if back:
            dz, dc = self.z - dz, self.cores - dc
        return ((zz + dz) % self.z) * self.cores + (cc + dc) % self.cores

    def row_peer(self, off):
        r, c = self.tp // self.cols, self.tp % self.cols
        return r * self.cols + (c + off) % self.cols

    def col_peer(self, off):
        r, c = self.tp // self.cols, self.tp % self.cols
        return ((r + off) % self.rows) * self.cols + c

    def tp_peer(self, off):
        return (self.tp + off) % self.n_tp


def send(src, dst, send_sem, recv_sem, sp, tp):
    copy = pltpu.make_async_remote_copy(
        src_ref=src, dst_ref=dst, send_sem=send_sem, recv_sem=recv_sem,
        device_id=(sp, tp), device_id_type=MESH,
    )
    copy.start()


def wait_bytes(ref, sem):
    pltpu.make_async_copy(ref, ref, sem).wait()


def meet(here):
    barrier = pltpu.get_barrier_semaphore()
    for place in here.order:
        pl.semaphore_signal(
            barrier, inc=1, device_id=(here.sp_peer(place), here.tp), device_id_type=MESH
        )
    for off in range(1, here.n_tp):
        pl.semaphore_signal(
            barrier, inc=1, device_id=(here.sp, here.tp_peer(off)), device_id_type=MESH
        )
    pl.semaphore_wait(barrier, here.n_sp + here.n_tp - 2)


def at(start, size):
    return pl.ds(pl.multiple_of(start * size, size), size)


def dispatch_kernel(
    n_sp, n_tp, routed, rows_in, mixer, out_routed, out_rows, mixer_all,
    sp_send, sp_recv, one_send, one_recv, two_send, two_recv, mix_send, mix_recv,
):
    here = Place(n_sp, n_tp)
    cap, width = routed.shape[0] // n_sp, routed.shape[1]
    tok = mixer.shape[0]
    meet(here)
    pairs = ((0, routed, out_routed), (1, rows_in, out_rows))
    for a, src, dst in pairs:
        for k, place in enumerate(here.order):
            peer = here.sp_peer(place)
            send(
                src.at[at(peer, cap)], dst.at[at(here.sp, cap), at(here.tp, width)],
                sp_send.at[a], sp_recv.at[a, k], peer, here.tp,
            )

    def spread(a, k, source, block, dst):
        firsts = range(1, here.cols if a == 0 else here.rows)
        seconds = range(1, here.rows if a == 0 else here.cols)
        first_peer = here.row_peer if a == 0 else here.col_peer
        second_peer = here.col_peer if a == 0 else here.row_peer
        target = dst.at[at(source, cap), at(here.tp, width)]
        for off in firsts:
            send(
                block, target, one_send.at[a], one_recv.at[a, k, off - 1],
                here.sp, first_peer(off),
            )
        for off in seconds:
            send(block, target, two_send.at[a], two_recv.at[a], here.sp, second_peer(off))

    def relay(a, k, source, dst):
        firsts = range(1, here.cols if a == 0 else here.rows)
        seconds = range(1, here.rows if a == 0 else here.cols)
        first_peer = here.row_peer if a == 0 else here.col_peer
        second_peer = here.col_peer if a == 0 else here.row_peer
        size = here.cols if a == 0 else here.rows
        for off in firsts:
            block = dst.at[at(source, cap), at(first_peer(size - off), width)]
            wait_bytes(block, one_recv.at[a, k, off - 1])
            for soff in seconds:
                send(block, block, two_send.at[a], two_recv.at[a], here.sp, second_peer(soff))

    last = len(here.order)
    for a, src, dst in pairs:
        spread(a, last, here.sp, src.at[at(here.sp, cap)], dst)
    for place in here.order:
        send(
            mixer, mixer_all.at[at(here.sp, tok)], mix_send.at[0], mix_recv.at[0],
            here.sp_peer(place), here.tp,
        )
    for a, src, dst in pairs:
        dst[at(here.sp, cap), at(here.tp, width)] = src[at(here.sp, cap), :]
    mixer_all[at(here.sp, tok), :] = mixer[...]
    sources = [here.sp_peer(place, back=True) for place in here.order] + [here.sp]
    steps = [last] + list(range(last))
    for i, k in enumerate(steps):
        if i + 1 < len(steps):
            k_next = steps[i + 1]
            for a, src, dst in pairs:
                block = dst.at[at(sources[k_next], cap), at(here.tp, width)]
                wait_bytes(block, sp_recv.at[a, k_next])
                spread(a, k_next, sources[k_next], block, dst)
        for a, src, dst in pairs:
            relay(a, k, sources[k], dst)
    for a, src, dst in pairs:
        count = here.cols - 1 if a == 0 else here.rows - 1
        twos = (here.rows - 1 if a == 0 else here.cols - 1) * (1 + count)
        wait_bytes(dst.at[:, pl.ds(0, twos * width)], two_recv.at[a])
        wait_bytes(dst.at[:, pl.ds(0, twos * width)], two_send.at[a])
        wait_bytes(dst.at[:, pl.ds(0, count * width)], one_send.at[a])
        wait_bytes(src.at[pl.ds(0, (n_sp - 1) * cap)], sp_send.at[a])
    wait_bytes(mixer_all.at[pl.ds(0, (n_sp - 1) * tok)], mix_recv.at[0])
    wait_bytes(mixer_all.at[pl.ds(0, (n_sp - 1) * tok)], mix_send.at[0])


def mm(a, b, ca, cb, precision=HIGHEST):
    return lax.dot_general(
        a, b, (((ca,), (cb,)), ((), ())), precision=precision, preferred_element_type=F32
    )


def triangle(size, lower):
    rows = lax.broadcasted_iota(jnp.int32, (size, size), 0)
    cols = lax.broadcasted_iota(jnp.int32, (size, size), 1)
    return rows >= cols if lower else rows <= cols


def return_kernel(
    n_sp, n_tp, parts, picker, cotangent, out_weight, queries, keys, values, decay, mixer_all,
    proj, grad_q, grad_k, grad_v, grad_l,
    got, summed, returned, piece, piece_t, pieces, carry, carries, total, totals, back, backs,
    state,
    tp_send, tp_recv, sp_send, sp_recv, piece_send, piece_recv, carry_send, carry_recv,
    total_send, total_recv, back_send, back_recv, res_send, res_recv,
):
    here = Place(n_sp, n_tp)
    me = here.sp
    cap, width = parts.shape[0] // n_sp, cotangent.shape[1]
    tok, blocks = queries.shape[0], queries.shape[0] // BLK
    out_rows = proj.shape[0]
    meet(here)
    order = list(reversed(here.order))
    for k, place in enumerate(order):
        peer = here.sp_peer(place)
        for off in range(1, n_tp):
            send(
                parts.at[at(peer, cap), at(here.tp_peer(off), width)],
                got.at[off - 1, at(peer, cap)],
                tp_send.at[0], tp_recv.at[k], me, here.tp_peer(off),
            )
    for off in range(1, n_tp):
        send(
            parts.at[at(me, cap), at(here.tp_peer(off), width)],
            got.at[off - 1, at(me, cap)],
            tp_send.at[0], tp_recv.at[n_sp - 1], me, here.tp_peer(off),
        )

    scale = DK ** (-0.5)
    lower = triangle(BLK, True)
    ones = jnp.where(lower, 1.0, 0.0).astype(F32)
    cums, ends = [], []
    for b in range(blocks):
        cum = mm(ones, decay[b * BLK:(b + 1) * BLK, :], 1, 0)
        cums.append(cum)
        ends.append(cum[BLK - 1:BLK, :])
    span = sum(ends[1:], ends[0])
    term = None
    for b in range(blocks):
        rows = slice(b * BLK, (b + 1) * BLK)
        key_end = keys[rows, :].astype(F32) * jnp.exp(ends[b] - cums[b])
        fresh = mm(values[rows, :].astype(F32), key_end, 0, 0)
        term = fresh if term is None else jnp.exp(ends[b]) * term + fresh
    carry[...] = term.astype(BF16)
    total[...] = jnp.broadcast_to(span, total.shape)
    for k, place in enumerate(here.order):
        peer = here.sp_peer(place)
        send(
            total, totals.at[me], total_send.at[0], total_recv.at[0], peer, here.tp
        )

        @pl.when(peer > me)
        def _():
            send(carry, carries.at[me], carry_send.at[k], carry_recv.at[k], peer, here.tp)

    for k, place in enumerate(order + [None]):
        source = me if place is None else here.sp_peer(place)
        wait_bytes(got.at[:, at(source, cap)], tp_recv.at[k])
        value = parts[at(source, cap), at(here.tp, width)].astype(F32)
        for off in range(1, n_tp):
            value = value + got[off - 1, at(source, cap), :].astype(F32)
        if place is None:
            returned[at(me, cap), :] = value.astype(BF16)
        else:
            summed[at(source, cap), :] = value.astype(BF16)
            send(
                summed.at[at(source, cap)], returned.at[at(me, cap)],
                sp_send.at[0], sp_recv.at[0], source, here.tp,
            )
    wait_bytes(returned.at[pl.ds(0, (n_sp - 1) * cap)], sp_recv.at[0])
    rowgrad = jnp.dot(picker[...], returned[...], preferred_element_type=F32)
    residual = (cotangent[...].astype(F32) + rowgrad).astype(BF16)
    piece[:, at(here.tp, width)] = residual
    for off in range(1, n_tp):
        send(
            piece.at[:, at(here.tp, width)], piece.at[:, at(here.tp, width)],
            piece_send.at[0], piece_recv.at[0], me, here.tp_peer(off),
        )

    wait_bytes(totals.at[pl.ds(0, n_sp - 1)], total_recv.at[0])
    totals[me] = total[...]
    for k, place in enumerate(here.order):
        source = here.sp_peer(place, back=True)

        @pl.when(source < me)
        def _():
            wait_bytes(carry, carry_recv.at[k])

    state[...] = jnp.zeros_like(state)
    for s in range(n_sp):
        @pl.when(s < me)
        def _():
            state[...] = jnp.exp(totals[s, 0:1, :]) * state[...] + carries[s].astype(F32)

    states = [state[...]]
    for b in range(blocks):
        rows = slice(b * BLK, (b + 1) * BLK)
        key_end = keys[rows, :].astype(F32) * jnp.exp(ends[b] - cums[b])
        states.append(
            jnp.exp(ends[b]) * states[b] + mm(values[rows, :].astype(F32), key_end, 0, 0)
        )

    wait_bytes(piece.at[:, pl.ds(0, (n_tp - 1) * width)], piece_recv.at[0])
    whole = piece[...]
    mix = jnp.dot(whole, out_weight[...], preferred_element_type=F32).astype(BF16).astype(F32)
    term = None
    for b in reversed(range(blocks)):
        rows = slice(b * BLK, (b + 1) * BLK)
        query_dec = queries[rows, :].astype(F32) * (scale * jnp.exp(cums[b]))
        fresh = mm(mix[rows, :], query_dec, 0, 0)
        term = fresh if term is None else jnp.exp(ends[b]) * term + fresh
    back[...] = term.astype(BF16)
    for k, place in enumerate(here.order):
        peer = here.sp_peer(place)

        @pl.when(peer < me)
        def _():
            send(back, backs.at[me], back_send.at[k], back_recv.at[k], peer, here.tp)

    piece_t[...] = whole.T
    for place in here.order:
        peer = here.sp_peer(place)
        send(
            piece_t.at[at(peer, out_rows)], pieces.at[me],
            res_send.at[0], res_recv.at[0], peer, here.tp,
        )

    kept = []
    for b in range(blocks):
        rows = slice(b * BLK, (b + 1) * BLK)
        grow, shrink = jnp.exp(cums[b]), jnp.exp(-cums[b])
        query_dec = queries[rows, :].astype(F32) * (scale * grow)
        key_dec = keys[rows, :].astype(F32) * shrink
        value, d_out = values[rows, :].astype(F32), mix[rows, :]
        scores = jnp.where(lower, mm(query_dec, key_dec, 1, 1), 0.0)
        d_scores = jnp.where(lower, mm(d_out, value, 1, 1), 0.0)
        d_query = (scale * grow) * (mm(d_out, states[b], 1, 0) + mm(d_scores, key_dec, 1, 0))
        d_key = shrink * mm(d_scores, query_dec, 0, 0)
        d_value = mm(scores, d_out, 0, 0)
        grad_q[rows, :] = d_query.astype(BF16)
        kept.append((d_query, d_key, d_value))

    for k, place in enumerate(here.order):
        source = here.sp_peer(place, back=True)

        @pl.when(source > me)
        def _():
            wait_bytes(back, back_recv.at[k])

    state[...] = jnp.zeros_like(state)
    for s in reversed(range(n_sp)):
        @pl.when(s > me)
        def _():
            state[...] = jnp.exp(totals[s, 0:1, :]) * state[...] + backs[s].astype(F32)

    leaving = state[...]
    edge = jnp.sum(states[blocks] * leaving, axis=0, keepdims=True)
    terms = [None] * blocks
    for b in reversed(range(blocks)):
        rows = slice(b * BLK, (b + 1) * BLK)
        query, key, value = queries[rows, :].astype(F32), keys[rows, :].astype(F32), values[rows, :].astype(F32)
        fall = jnp.exp(ends[b] - cums[b])
        d_query, d_key, d_value = kept[b]
        d_key = d_key + fall * mm(value, leaving, 1, 0)
        d_value = d_value + mm(key * fall, leaving, 1, 1)
        grad_k[rows, :] = d_key.astype(BF16)
        grad_v[rows, :] = d_value.astype(BF16)
        terms[b] = query * d_query - key * d_key
        if b:
            query_dec = query * (scale * jnp.exp(cums[b]))
            leaving = jnp.exp(ends[b]) * leaving + mm(mix[rows, :], query_dec, 0, 0)
    upper = jnp.where(triangle(BLK, False), 1.0, 0.0).astype(F32)
    for b in reversed(range(blocks)):
        rows = slice(b * BLK, (b + 1) * BLK)
        grad_l[rows, :] = mm(upper, terms[b], 1, 0) + edge
        edge = edge + jnp.sum(terms[b], axis=0, keepdims=True)

    wait_bytes(pieces.at[pl.ds(0, n_sp - 1)], res_recv.at[0])
    pieces[me] = piece_t[at(me, out_rows), :]
    acc = jnp.zeros(proj.shape, F32)
    for s in range(n_sp):
        acc = acc + jnp.dot(
            pieces[s], mixer_all[s * tok:(s + 1) * tok, :], preferred_element_type=F32
        )
    proj[...] = acc

    wait_bytes(got, tp_send.at[0])
    wait_bytes(returned.at[pl.ds(0, (n_sp - 1) * cap)], sp_send.at[0])
    wait_bytes(piece.at[:, pl.ds(0, (n_tp - 1) * width)], piece_send.at[0])
    wait_bytes(totals.at[pl.ds(0, n_sp - 1)], total_send.at[0])
    wait_bytes(pieces.at[pl.ds(0, n_sp - 1)], res_send.at[0])
    for k, place in enumerate(here.order):
        peer = here.sp_peer(place)

        @pl.when(peer > me)
        def _():
            wait_bytes(carry, carry_send.at[k])

        @pl.when(peer < me)
        def _():
            wait_bytes(back, back_send.at[k])


def vmem():
    return pl.BlockSpec(memory_space=pltpu.VMEM)


def shards(
    n_sp, n_tp,
    cotangent, moe_input, expert_ids, group_gate, expert_gate, weight_gate, weight_up,
    weight_down, out_weight, mixer_out, queries, key_vectors, values, log_decay,
):
    tokens, width = cotangent.shape
    width_d = width * n_tp
    experts = n_sp
    capacity = -(-max(2, 3 * TOK // experts) // 16) * 16
    slots = experts * capacity
    flat_ids = expert_ids.reshape(-1)
    onehot = (flat_ids[:, None] == jnp.arange(experts, dtype=jnp.int32)[None, :]).astype(jnp.int32)
    before = jnp.cumsum(onehot, axis=0) - onehot
    position = jnp.sum(before * onehot, axis=1)
    slot_index = flat_ids * capacity + position
    slot_match = slot_index[:, None] == jnp.arange(slots, dtype=jnp.int32)[None, :]
    route_weight = (group_gate[:, None] * expert_gate).reshape(-1)
    slot_weight = jnp.sum(jnp.where(slot_match, route_weight[:, None], 0.0), axis=0)
    picker = jnp.any(slot_match.reshape(tokens, 2, -1), axis=1).astype(BF16)
    contract = (((0,), (0,)), ((), ()))
    pulled_grad = lax.dot_general(picker, cotangent, contract, preferred_element_type=F32)
    rows_in = lax.dot_general(picker, moe_input, contract, preferred_element_type=F32).astype(BF16)
    routed = (slot_weight[:, None] * pulled_grad).astype(BF16)

    dma, rows_tp, cols_tp = pltpu.SemaphoreType.DMA, *tp_grid(n_tp)
    ones = max(rows_tp, cols_tp) - 1
    routed, rows_in, mixer_all = pl.pallas_call(
        functools.partial(dispatch_kernel, n_sp, n_tp),
        out_shape=(
            jax.ShapeDtypeStruct((slots, width_d), BF16),
            jax.ShapeDtypeStruct((slots, width_d), BF16),
            jax.ShapeDtypeStruct((n_sp * tokens, DV), BF16),
        ),
        in_specs=[vmem()] * 3,
        out_specs=(vmem(),) * 3,
        scratch_shapes=[
            dma((2,)), dma((2, n_sp)), dma((2,)), dma((2, n_sp, ones)),
            dma((2,)), dma((2,)), dma((1,)), dma((1,)),
        ],
        compiler_params=pltpu.CompilerParams(collective_id=0, has_side_effects=True),
        name="dispatch",
    )(routed, rows_in, mixer_out)

    w_gate, w_up, w_down = (weight_gate[0], weight_up[0], weight_down[0])
    gate_pre = jnp.dot(rows_in, w_gate, preferred_element_type=F32)
    up_pre = jnp.dot(rows_in, w_up, preferred_element_type=F32)
    sigmoid_g = jax.nn.sigmoid(gate_pre)
    active = gate_pre * sigmoid_g
    hidden = (active * up_pre).astype(BF16)
    across = (((1,), (1,)), ((), ()))
    back_grad = lax.dot_general(routed, w_down, across, preferred_element_type=F32)
    d_up = (back_grad * active).astype(BF16)
    d_gate = (back_grad * up_pre * sigmoid_g * (1.0 + gate_pre * (1.0 - sigmoid_g))).astype(BF16)
    grad_down = lax.dot_general(hidden, routed, contract, preferred_element_type=F32).astype(BF16)
    grad_gate = lax.dot_general(rows_in, d_gate, contract, preferred_element_type=F32).astype(BF16)
    grad_up = lax.dot_general(rows_in, d_up, contract, preferred_element_type=F32).astype(BF16)
    parts = lax.dot_general(d_gate, w_gate, across, preferred_element_type=F32)
    parts = parts + lax.dot_general(d_up, w_up, across, preferred_element_type=F32)
    parts = parts.astype(BF16)

    out_rows = width_d // n_sp
    proj, grad_q, grad_k, grad_v, grad_l = pl.pallas_call(
        functools.partial(return_kernel, n_sp, n_tp),
        out_shape=(
            jax.ShapeDtypeStruct((out_rows, DV), F32),
            jax.ShapeDtypeStruct((tokens, DK), BF16),
            jax.ShapeDtypeStruct((tokens, DK), BF16),
            jax.ShapeDtypeStruct((tokens, DV), BF16),
            jax.ShapeDtypeStruct((tokens, DK), F32),
        ),
        in_specs=[vmem()] * 9,
        out_specs=(vmem(),) * 5,
        scratch_shapes=[
            pltpu.VMEM((n_tp - 1, slots, width), BF16),
            pltpu.VMEM((slots, width), BF16),
            pltpu.VMEM((slots, width), BF16),
            pltpu.VMEM((tokens, width_d), BF16),
            pltpu.VMEM((width_d, tokens), BF16),
            pltpu.VMEM((n_sp, out_rows, tokens), BF16),
            pltpu.VMEM((DV, DK), BF16),
            pltpu.VMEM((n_sp, DV, DK), BF16),
            pltpu.VMEM((8, DK), F32),
            pltpu.VMEM((n_sp, 8, DK), F32),
            pltpu.VMEM((DV, DK), BF16),
            pltpu.VMEM((n_sp, DV, DK), BF16),
            pltpu.VMEM((DV, DK), F32),
            dma((1,)), dma((n_sp,)), dma((1,)), dma((1,)), dma((1,)), dma((1,)),
            dma((n_sp,)), dma((n_sp,)), dma((1,)), dma((1,)),
            dma((n_sp,)), dma((n_sp,)), dma((1,)), dma((1,)),
        ],
        compiler_params=pltpu.CompilerParams(collective_id=1, has_side_effects=True),
        name="combine",
    )(parts, picker, cotangent, out_weight, queries, key_vectors, values, log_decay, mixer_all)
    return (
        grad_gate[None], grad_up[None], grad_down[None], proj, grad_q, grad_k, grad_v, grad_l,
    )


def solution(mesh):
    n_sp, n_tp = mesh.shape["sp"], mesh.shape["tp"]
    return jax.shard_map(
        functools.partial(shards, n_sp, n_tp),
        mesh=mesh,
        in_specs=(
            P("sp", "tp"), P("sp", "tp"), P("sp", None), P("sp"), P("sp", None),
            P("sp", None, "tp"), P("sp", None, "tp"), P("sp", "tp", None), P(None, "tp"),
            P("sp", "tp"), P("sp", "tp"), P("sp", "tp"), P("sp", "tp"), P("sp", "tp"),
        ),
        out_specs=(
            P("sp", None, "tp"), P("sp", None, "tp"), P("sp", "tp", None),
            P("sp", "tp"), P("sp", "tp"), P("sp", "tp"), P("sp", "tp"), P("sp", "tp"),
        ),
        check_vma=False,
    )
```

```python
import functools
import math

import jax
import jax.numpy as jnp
from jax import lax
from jax.experimental import pallas as pl
from jax.experimental.pallas import tpu as pltpu
from jax.sharding import PartitionSpec as P

DK = 128
DV = 256
TOK = 128
BLK = 64
HIGHEST = lax.Precision.HIGHEST
F32 = jnp.float32
BF16 = jnp.bfloat16
MESH = pl.DeviceIdType.MESH


def tp_grid(n_tp):
    cols = math.isqrt(n_tp)
    while n_tp % cols:
        cols -= 1
    return n_tp // cols, cols


def sp_order(n_sp):
    z = n_sp // 2
    places = [(dz, dc) for dz in range(z) for dc in range(2)][1:]
    places.sort(key=lambda p: (min(p[0], z - p[0]), p))
    return places, z, 2


class Place:
    def __init__(self, n_sp, n_tp):
        self.n_sp, self.n_tp = n_sp, n_tp
        self.sp, self.tp = lax.axis_index("sp"), lax.axis_index("tp")
        self.order, self.z, self.cores = sp_order(n_sp)
        self.rows, self.cols = tp_grid(n_tp)
        self.chip, self.core = self.sp // self.cores, self.sp % self.cores
        self.chips = sorted(range(1, self.z), key=lambda dz: (min(dz, self.z - dz), dz))

    def sp_peer(self, place, back=False):
        dz, dc = place
        zz, cc = self.sp // self.cores, self.sp % self.cores
        if back:
            dz, dc = self.z - dz, self.cores - dc
        return ((zz + dz) % self.z) * self.cores + (cc + dc) % self.cores

    def row_peer(self, off):
        r, c = self.tp // self.cols, self.tp % self.cols
        return r * self.cols + (c + off) % self.cols

    def col_peer(self, off):
        r, c = self.tp // self.cols, self.tp % self.cols
        return ((r + off) % self.rows) * self.cols + c

    def tp_peer(self, off):
        return (self.tp + off) % self.n_tp


def send(src, dst, send_sem, recv_sem, sp, tp):
    copy = pltpu.make_async_remote_copy(
        src_ref=src, dst_ref=dst, send_sem=send_sem, recv_sem=recv_sem,
        device_id=(sp, tp), device_id_type=MESH,
    )
    copy.start()


def wait_bytes(ref, sem):
    pltpu.make_async_copy(ref, ref, sem).wait()


def greet(here):
    barrier = pltpu.get_barrier_semaphore()
    for place in here.order:
        pl.semaphore_signal(
            barrier, inc=1, device_id=(here.sp_peer(place), here.tp), device_id_type=MESH
        )
    for off in range(1, here.n_tp):
        pl.semaphore_signal(
            barrier, inc=1, device_id=(here.sp, here.tp_peer(off)), device_id_type=MESH
        )


def greeted(here):
    pl.semaphore_wait(pltpu.get_barrier_semaphore(), here.n_sp + here.n_tp - 2)


def meet(here):
    greet(here)
    greeted(here)


def pull(picker, rows):
    return lax.dot_general(picker, rows, (((0,), (0,)), ((), ())), preferred_element_type=F32)


def at(start, size):
    return pl.ds(pl.multiple_of(start * size, size), size)


def dispatch_kernel(
    n_sp, n_tp, picker, weight, cotangent, moe_input, mixer, out_routed, out_rows, mixer_all,
    routed, rows_in,
    sp_send, sp_recv, one_send, one_recv, two_send, two_recv, mix_send, mix_recv,
    pair_send, pair_recv,
):
    here = Place(n_sp, n_tp)
    cap, width = routed.shape[0] // n_sp, routed.shape[1]
    tok = mixer.shape[0]
    greet(here)
    chosen = picker[...]
    routed[...] = (weight[...] * pull(chosen, cotangent[...])).astype(BF16)
    rows_in[...] = pull(chosen, moe_input[...]).astype(BF16)
    greeted(here)
    pairs = ((0, routed, out_routed), (1, rows_in, out_rows))
    for k, place in enumerate(here.order):
        peer = here.sp_peer(place)
        for a, src, dst in pairs:
            send(
                src.at[at(peer, cap)], dst.at[at(here.sp, cap), at(here.tp, width)],
                sp_send.at[a], sp_recv.at[a, k], peer, here.tp,
            )

    def spread(a, k, source, block, dst):
        firsts = range(1, here.cols if a == 0 else here.rows)
        seconds = range(1, here.rows if a == 0 else here.cols)
        first_peer = here.row_peer if a == 0 else here.col_peer
        second_peer = here.col_peer if a == 0 else here.row_peer
        target = dst.at[at(source, cap), at(here.tp, width)]
        for off in firsts:
            send(
                block, target, one_send.at[a], one_recv.at[a, k, off - 1],
                here.sp, first_peer(off),
            )
        for off in seconds:
            send(block, target, two_send.at[a], two_recv.at[a], here.sp, second_peer(off))

    def relay(a, k, source, dst):
        firsts = range(1, here.cols if a == 0 else here.rows)
        seconds = range(1, here.rows if a == 0 else here.cols)
        first_peer = here.row_peer if a == 0 else here.col_peer
        second_peer = here.col_peer if a == 0 else here.row_peer
        size = here.cols if a == 0 else here.rows
        for off in firsts:
            block = dst.at[at(source, cap), at(first_peer(size - off), width)]
            wait_bytes(block, one_recv.at[a, k, off - 1])
            for soff in seconds:
                send(block, block, two_send.at[a], two_recv.at[a], here.sp, second_peer(soff))

    last = len(here.order)
    for a, src, dst in pairs:
        spread(a, last, here.sp, src.at[at(here.sp, cap)], dst)
    mate = here.sp_peer((0, 1))
    mine = mixer_all.at[at(here.sp, tok)]
    send(mixer, mine, pair_send.at[0], pair_recv.at[0], mate, here.tp)
    for dz in here.chips:
        send(
            mixer, mine, mix_send.at[0], mix_recv.at[dz], here.sp_peer((dz, 0)), here.tp
        )
    for a, src, dst in pairs:
        dst[at(here.sp, cap), at(here.tp, width)] = src[at(here.sp, cap), :]
    mixer_all[at(here.sp, tok), :] = mixer[...]
    sources = [here.sp_peer(place, back=True) for place in here.order] + [here.sp]
    steps = [last] + list(range(last))
    for i, k in enumerate(steps):
        if i + 1 < len(steps):
            k_next = steps[i + 1]
            for a, src, dst in pairs:
                block = dst.at[at(sources[k_next], cap), at(here.tp, width)]
                wait_bytes(block, sp_recv.at[a, k_next])
                spread(a, k_next, sources[k_next], block, dst)
        for a, src, dst in pairs:
            relay(a, k, sources[k], dst)
    for dz in here.chips:
        block = mixer_all.at[at(here.sp_peer((dz, 0), back=True), tok)]
        wait_bytes(block, mix_recv.at[dz])
        send(block, block, pair_send.at[0], pair_recv.at[0], mate, here.tp)
    for a, src, dst in pairs:
        count = here.cols - 1 if a == 0 else here.rows - 1
        twos = (here.rows - 1 if a == 0 else here.cols - 1) * (1 + count)
        wait_bytes(dst.at[:, pl.ds(0, twos * width)], two_recv.at[a])
        wait_bytes(dst.at[:, pl.ds(0, twos * width)], two_send.at[a])
        wait_bytes(dst.at[:, pl.ds(0, count * width)], one_send.at[a])
        wait_bytes(src.at[pl.ds(0, (n_sp - 1) * cap)], sp_send.at[a])
    wait_bytes(mixer_all.at[pl.ds(0, (here.z - 1) * tok)], mix_send.at[0])
    wait_bytes(mixer_all.at[pl.ds(0, here.z * tok)], pair_recv.at[0])
    wait_bytes(mixer_all.at[pl.ds(0, here.z * tok)], pair_send.at[0])


def mm(a, b, ca, cb, precision=HIGHEST):
    return lax.dot_general(
        a, b, (((ca,), (cb,)), ((), ())), precision=precision, preferred_element_type=F32
    )


def triangle(size, lower):
    rows = lax.broadcasted_iota(jnp.int32, (size, size), 0)
    cols = lax.broadcasted_iota(jnp.int32, (size, size), 1)
    return rows >= cols if lower else rows <= cols


def return_kernel(
    n_sp, n_tp, parts, picker, cotangent, out_weight, queries, keys, values, decay, mixer_all,
    proj, grad_q, grad_k, grad_v, grad_l,
    got, summed, returned, piece, piece_t, pieces, own, other, half, halves, total, totals,
    state, edges,
    tp_send, tp_recv, sp_send, sp_recv, piece_send, piece_recv, mate_send, mate_recv,
    half_send, half_recv, edge_send, edge_recv, total_send, total_recv, res_send, res_recv,
):
    here = Place(n_sp, n_tp)
    me = here.sp
    cap, width = parts.shape[0] // n_sp, cotangent.shape[1]
    tok, blocks = queries.shape[0], queries.shape[0] // BLK
    out_rows = proj.shape[0]
    meet(here)
    order = list(reversed(here.order))
    for k, place in enumerate(order):
        peer = here.sp_peer(place)
        for off in range(1, n_tp):
            send(
                parts.at[at(peer, cap), at(here.tp_peer(off), width)],
                got.at[off - 1, at(peer, cap)],
                tp_send.at[0], tp_recv.at[k], me, here.tp_peer(off),
            )
    for off in range(1, n_tp):
        send(
            parts.at[at(me, cap), at(here.tp_peer(off), width)],
            got.at[off - 1, at(me, cap)],
            tp_send.at[0], tp_recv.at[n_sp - 1], me, here.tp_peer(off),
        )

    scale = DK ** (-0.5)
    lower = triangle(BLK, True)
    ones = jnp.where(lower, 1.0, 0.0).astype(F32)
    cums, ends = [], []
    for b in range(blocks):
        cum = mm(ones, decay[b * BLK:(b + 1) * BLK, :], 1, 0)
        cums.append(cum)
        ends.append(cum[BLK - 1:BLK, :])
    span = sum(ends[1:], ends[0])
    term = None
    for b in range(blocks):
        rows = slice(b * BLK, (b + 1) * BLK)
        key_end = keys[rows, :].astype(F32) * jnp.exp(ends[b] - cums[b])
        fresh = mm(values[rows, :].astype(F32), key_end, 0, 0)
        term = fresh if term is None else jnp.exp(ends[b]) * term + fresh
    own[0] = term.astype(BF16)
    total[...] = jnp.broadcast_to(span, total.shape)
    mate = here.sp_peer((0, 1))
    first_core = here.core == 0
    rows_half = half.shape[1]
    send(own.at[0], other.at[0], mate_send.at[0], mate_recv.at[0], mate, here.tp)
    for place in here.order:
        send(
            total, totals.at[me], total_send.at[0], total_recv.at[0],
            here.sp_peer(place), here.tp,
        )

    def in_order(way):
        mine, theirs = own[way].astype(F32), other[way].astype(F32)
        return jnp.where(first_core, mine, theirs), jnp.where(first_core, theirs, mine)

    def share(way):
        wait_bytes(other.at[way], mate_recv.at[way])
        early, late = in_order(way)
        here_early = jnp.exp(totals[here.chip * 2, 0:1, :])
        here_late = jnp.exp(totals[here.chip * 2 + 1, 0:1, :])
        chip = (here_late * early + late) if way == 0 else (early + here_early * late)
        half[way] = jnp.where(first_core, chip[:rows_half], chip[rows_half:]).astype(BF16)
        for dz in here.chips:
            far = (here.chip + dz) % here.z
            needed = (far > here.chip) if way == 0 else (far < here.chip)

            @pl.when(needed)
            def _():
                send(
                    half.at[way], halves.at[way, here.chip], half_send.at[way, dz],
                    half_recv.at[way, dz], here.sp_peer((dz, 0)), here.tp,
                )

    def settle(way):
        for dz in here.chips:
            far = (here.chip + here.z - dz) % here.z
            needed = (far < here.chip) if way == 0 else (far > here.chip)

            @pl.when(needed)
            def _():
                wait_bytes(half.at[way], half_recv.at[way, dz])

        state[...] = jnp.zeros_like(state)
        for z in range(here.z) if way == 0 else reversed(range(here.z)):
            @pl.when((z < here.chip) if way == 0 else (z > here.chip))
            def _():
                decays = jnp.exp(totals[2 * z, 0:1, :] + totals[2 * z + 1, 0:1, :])
                state[...] = decays * state[...] + halves[way, z].astype(F32)

        edges[way, here.core] = state[...]
        send(
            edges.at[way, here.core], edges.at[way, here.core],
            edge_send.at[way], edge_recv.at[way], mate, here.tp,
        )
        wait_bytes(state, edge_recv.at[way])
        chip_edge = jnp.concatenate([edges[way, 0], edges[way, 1]], axis=0)
        early, late = in_order(way)
        if way == 0:
            passed = jnp.exp(totals[here.chip * 2, 0:1, :]) * chip_edge + early
            return jnp.where(first_core, chip_edge, passed)
        passed = jnp.exp(totals[here.chip * 2 + 1, 0:1, :]) * chip_edge + late
        return jnp.where(first_core, passed, chip_edge)

    wait_bytes(totals.at[pl.ds(0, n_sp - 1)], total_recv.at[0])
    totals[me] = total[...]
    share(0)
    for k, place in enumerate(order + [None]):
        source = me if place is None else here.sp_peer(place)
        wait_bytes(got.at[:, at(source, cap)], tp_recv.at[k])
        value = parts[at(source, cap), at(here.tp, width)].astype(F32)
        for off in range(1, n_tp):
            value = value + got[off - 1, at(source, cap), :].astype(F32)
        if place is None:
            returned[at(me, cap), :] = value.astype(BF16)
        else:
            summed[at(source, cap), :] = value.astype(BF16)
            send(
                summed.at[at(source, cap)], returned.at[at(me, cap)],
                sp_send.at[0], sp_recv.at[0], source, here.tp,
            )
    wait_bytes(returned.at[pl.ds(0, (n_sp - 1) * cap)], sp_recv.at[0])
    rowgrad = jnp.dot(picker[...], returned[...], preferred_element_type=F32)
    residual = (cotangent[...].astype(F32) + rowgrad).astype(BF16)
    piece[:, at(here.tp, width)] = residual
    for off in range(1, n_tp):
        send(
            piece.at[:, at(here.tp, width)], piece.at[:, at(here.tp, width)],
            piece_send.at[0], piece_recv.at[0], me, here.tp_peer(off),
        )

    states = [settle(0)]
    for b in range(blocks):
        rows = slice(b * BLK, (b + 1) * BLK)
        key_end = keys[rows, :].astype(F32) * jnp.exp(ends[b] - cums[b])
        states.append(
            jnp.exp(ends[b]) * states[b] + mm(values[rows, :].astype(F32), key_end, 0, 0)
        )

    wait_bytes(piece.at[:, pl.ds(0, (n_tp - 1) * width)], piece_recv.at[0])
    whole = piece[...]
    mix = jnp.dot(whole, out_weight[...], preferred_element_type=F32).astype(BF16).astype(F32)
    term = None
    for b in reversed(range(blocks)):
        rows = slice(b * BLK, (b + 1) * BLK)
        query_dec = queries[rows, :].astype(F32) * (scale * jnp.exp(cums[b]))
        fresh = mm(mix[rows, :], query_dec, 0, 0)
        term = fresh if term is None else jnp.exp(ends[b]) * term + fresh
    own[1] = term.astype(BF16)
    send(own.at[1], other.at[1], mate_send.at[1], mate_recv.at[1], mate, here.tp)
    share(1)
    piece_t[...] = whole.T
    for place in here.order:
        peer = here.sp_peer(place)
        send(
            piece_t.at[at(peer, out_rows)], pieces.at[me],
            res_send.at[0], res_recv.at[0], peer, here.tp,
        )

    kept = []
    for b in range(blocks):
        rows = slice(b * BLK, (b + 1) * BLK)
        grow, shrink = jnp.exp(cums[b]), jnp.exp(-cums[b])
        query_dec = queries[rows, :].astype(F32) * (scale * grow)
        key_dec = keys[rows, :].astype(F32) * shrink
        value, d_out = values[rows, :].astype(F32), mix[rows, :]
        scores = jnp.where(lower, mm(query_dec, key_dec, 1, 1), 0.0)
        d_scores = jnp.where(lower, mm(d_out, value, 1, 1), 0.0)
        d_query = (scale * grow) * (mm(d_out, states[b], 1, 0) + mm(d_scores, key_dec, 1, 0))
        d_key = shrink * mm(d_scores, query_dec, 0, 0)
        d_value = mm(scores, d_out, 0, 0)
        grad_q[rows, :] = d_query.astype(BF16)
        kept.append((d_query, d_key, d_value))

    leaving = settle(1)
    edge = jnp.sum(states[blocks] * leaving, axis=0, keepdims=True)
    terms = [None] * blocks
    for b in reversed(range(blocks)):
        rows = slice(b * BLK, (b + 1) * BLK)
        query, key, value = queries[rows, :].astype(F32), keys[rows, :].astype(F32), values[rows, :].astype(F32)
        fall = jnp.exp(ends[b] - cums[b])
        d_query, d_key, d_value = kept[b]
        d_key = d_key + fall * mm(value, leaving, 1, 0)
        d_value = d_value + mm(key * fall, leaving, 1, 1)
        grad_k[rows, :] = d_key.astype(BF16)
        grad_v[rows, :] = d_value.astype(BF16)
        terms[b] = query * d_query - key * d_key
        if b:
            query_dec = query * (scale * jnp.exp(cums[b]))
            leaving = jnp.exp(ends[b]) * leaving + mm(mix[rows, :], query_dec, 0, 0)
    upper = jnp.where(triangle(BLK, False), 1.0, 0.0).astype(F32)
    for b in reversed(range(blocks)):
        rows = slice(b * BLK, (b + 1) * BLK)
        grad_l[rows, :] = mm(upper, terms[b], 1, 0) + edge
        edge = edge + jnp.sum(terms[b], axis=0, keepdims=True)

    wait_bytes(pieces.at[pl.ds(0, n_sp - 1)], res_recv.at[0])
    pieces[me] = piece_t[at(me, out_rows), :]
    acc = jnp.zeros(proj.shape, F32)
    for s in range(n_sp):
        acc = acc + jnp.dot(
            pieces[s], mixer_all[s * tok:(s + 1) * tok, :], preferred_element_type=F32
        )
    proj[...] = acc

    wait_bytes(got, tp_send.at[0])
    wait_bytes(returned.at[pl.ds(0, (n_sp - 1) * cap)], sp_send.at[0])
    wait_bytes(piece.at[:, pl.ds(0, (n_tp - 1) * width)], piece_send.at[0])
    wait_bytes(totals.at[pl.ds(0, n_sp - 1)], total_send.at[0])
    wait_bytes(pieces.at[pl.ds(0, n_sp - 1)], res_send.at[0])
    for way in range(2):
        wait_bytes(own.at[way], mate_send.at[way])
        wait_bytes(state, edge_send.at[way])
        for dz in here.chips:
            far = (here.chip + dz) % here.z

            @pl.when((far > here.chip) if way == 0 else (far < here.chip))
            def _():
                wait_bytes(half.at[way], half_send.at[way, dz])


def finish_kernel(*refs):
    count = len(refs) // 2
    for source, target in zip(refs[:count], refs[count:]):
        target[...] = source[...]


def vmem():
    return pl.BlockSpec(memory_space=pltpu.VMEM)


def shards(
    n_sp, n_tp,
    cotangent, moe_input, expert_ids, group_gate, expert_gate, weight_gate, weight_up,
    weight_down, out_weight, mixer_out, queries, key_vectors, values, log_decay,
):
    tokens, width = cotangent.shape
    width_d = width * n_tp
    experts = n_sp
    capacity = -(-max(2, 3 * TOK // experts) // 16) * 16
    slots = experts * capacity
    flat_ids = expert_ids.reshape(-1)
    onehot = (flat_ids[:, None] == jnp.arange(experts, dtype=jnp.int32)[None, :]).astype(jnp.int32)
    before = jnp.cumsum(onehot, axis=0) - onehot
    position = jnp.sum(before * onehot, axis=1)
    slot_index = flat_ids * capacity + position
    slot_match = slot_index[:, None] == jnp.arange(slots, dtype=jnp.int32)[None, :]
    route_weight = (group_gate[:, None] * expert_gate).reshape(-1)
    slot_weight = jnp.sum(jnp.where(slot_match, route_weight[:, None], 0.0), axis=0)
    picker = jnp.any(slot_match.reshape(tokens, 2, -1), axis=1).astype(BF16)
    contract = (((0,), (0,)), ((), ()))

    dma, rows_tp, cols_tp = pltpu.SemaphoreType.DMA, *tp_grid(n_tp)
    ones = max(rows_tp, cols_tp) - 1
    routed, rows_in, mixer_all = pl.pallas_call(
        functools.partial(dispatch_kernel, n_sp, n_tp),
        out_shape=(
            jax.ShapeDtypeStruct((slots, width_d), BF16),
            jax.ShapeDtypeStruct((slots, width_d), BF16),
            jax.ShapeDtypeStruct((n_sp * tokens, DV), BF16),
        ),
        in_specs=[vmem()] * 5,
        out_specs=(vmem(),) * 3,
        scratch_shapes=[
            pltpu.VMEM((slots, width), BF16), pltpu.VMEM((slots, width), BF16),
            dma((2,)), dma((2, n_sp)), dma((2,)), dma((2, n_sp, ones)),
            dma((2,)), dma((2,)), dma((1,)), dma((n_sp,)),
            dma((1,)), dma((1,)),
        ],
        compiler_params=pltpu.CompilerParams(collective_id=0, has_side_effects=True),
        name="dispatch",
    )(picker, slot_weight[:, None], cotangent, moe_input, mixer_out)

    w_gate, w_up, w_down = (weight_gate[0], weight_up[0], weight_down[0])
    gate_pre = jnp.dot(rows_in, w_gate, preferred_element_type=F32)
    up_pre = jnp.dot(rows_in, w_up, preferred_element_type=F32)
    sigmoid_g = jax.nn.sigmoid(gate_pre)
    active = gate_pre * sigmoid_g
    hidden = (active * up_pre).astype(BF16)
    across = (((1,), (1,)), ((), ()))
    back_grad = lax.dot_general(routed, w_down, across, preferred_element_type=F32)
    d_up = (back_grad * active).astype(BF16)
    d_gate = (back_grad * up_pre * sigmoid_g * (1.0 + gate_pre * (1.0 - sigmoid_g))).astype(BF16)
    grad_down = lax.dot_general(hidden, routed, contract, preferred_element_type=F32).astype(BF16)
    grad_gate = lax.dot_general(rows_in, d_gate, contract, preferred_element_type=F32).astype(BF16)
    grad_up = lax.dot_general(rows_in, d_up, contract, preferred_element_type=F32).astype(BF16)
    parts = lax.dot_general(d_gate, w_gate, across, preferred_element_type=F32)
    parts = parts + lax.dot_general(d_up, w_up, across, preferred_element_type=F32)
    parts = parts.astype(BF16)

    out_rows = width_d // n_sp
    shapes = (
        jax.ShapeDtypeStruct((out_rows, DV), F32),
        jax.ShapeDtypeStruct((tokens, DK), BF16),
        jax.ShapeDtypeStruct((tokens, DK), BF16),
        jax.ShapeDtypeStruct((tokens, DV), BF16),
        jax.ShapeDtypeStruct((tokens, DK), F32),
    )
    results = pl.pallas_call(
        functools.partial(return_kernel, n_sp, n_tp),
        out_shape=shapes,
        in_specs=[vmem()] * 9,
        out_specs=(vmem(),) * 5,
        scratch_shapes=[
            pltpu.VMEM((n_tp - 1, slots, width), BF16),
            pltpu.VMEM((slots, width), BF16),
            pltpu.VMEM((slots, width), BF16),
            pltpu.VMEM((tokens, width_d), BF16),
            pltpu.VMEM((width_d, tokens), BF16),
            pltpu.VMEM((n_sp, out_rows, tokens), BF16),
            pltpu.VMEM((2, DV, DK), BF16),
            pltpu.VMEM((2, DV, DK), BF16),
            pltpu.VMEM((2, DV // 2, DK), BF16),
            pltpu.VMEM((2, n_sp // 2, DV // 2, DK), BF16),
            pltpu.VMEM((8, DK), F32),
            pltpu.VMEM((n_sp, 8, DK), F32),
            pltpu.VMEM((DV // 2, DK), F32),
            pltpu.VMEM((2, 2, DV // 2, DK), F32),
            dma((1,)), dma((n_sp,)), dma((1,)), dma((1,)), dma((1,)), dma((1,)),
            dma((2,)), dma((2,)), dma((2, n_sp // 2)), dma((2, n_sp // 2)),
            dma((2,)), dma((2,)), dma((1,)), dma((1,)), dma((1,)), dma((1,)),
        ],
        compiler_params=pltpu.CompilerParams(collective_id=1, has_side_effects=True),
        name="combine",
    )(parts, picker, cotangent, out_weight, queries, key_vectors, values, log_decay, mixer_all)
    proj, grad_q, grad_k, grad_v, grad_l = pl.pallas_call(
        finish_kernel, out_shape=shapes, in_specs=[vmem()] * 5, out_specs=(vmem(),) * 5,
        name="finish",
    )(*results)
    return (
        grad_gate[None], grad_up[None], grad_down[None], proj, grad_q, grad_k, grad_v, grad_l,
    )


def solution(mesh):
    n_sp, n_tp = mesh.shape["sp"], mesh.shape["tp"]
    return jax.shard_map(
        functools.partial(shards, n_sp, n_tp),
        mesh=mesh,
        in_specs=(
            P("sp", "tp"), P("sp", "tp"), P("sp", None), P("sp"), P("sp", None),
            P("sp", None, "tp"), P("sp", None, "tp"), P("sp", "tp", None), P(None, "tp"),
            P("sp", "tp"), P("sp", "tp"), P("sp", "tp"), P("sp", "tp"), P("sp", "tp"),
        ),
        out_specs=(
            P("sp", None, "tp"), P("sp", None, "tp"), P("sp", "tp", None),
            P("sp", "tp"), P("sp", "tp"), P("sp", "tp"), P("sp", "tp"), P("sp", "tp"),
        ),
        check_vma=False,
    )
```
